256 devices in a mesh: sp: 64 (over z, x, core), tp: 4 (over y).
Axes of the slice: x: 4, y: 4, z: 8, core: 2. Of those that a mesh axis runs over, the one named last changes fastest.
Arguments:
- skip_connection_stream: bfloat16 [49152, 2048], P('sp'), may hold values from -6 to 6
- probing_vectors: bfloat16 [49152, 512], P('sp', 'tp'), may hold values from -6 to 6
- addressing_vectors: bfloat16 [49152, 512], P('sp', 'tp'), may hold values from -6 to 6
- mapped_payloads: bfloat16 [49152, 1024], P('sp', 'tp'), may hold values from -6 to 6
- emission_switch: bfloat16 [49152, 1024], P('sp', 'tp'), may hold values from -6 to 6
- lapse_preactivation: bfloat16 [49152, 512], P('sp', 'tp')
- lapse_shift_entries: float32 [512], P('tp')
- surplus_attenuation_terms: float32 [49152], P('sp'), may hold values from -0.7 to 0
- passage_label_per_token: int32 [49152], P('sp'), may hold values from 0 to 15, never falling along the last dimension, each value on 1 to 6144 neighbouring positions
- attention_group_rescaler: float32 [128], replicated, may hold values from 0.1 to 1.9
- emission_projector: bfloat16 [1024, 2048], P('tp'), may hold values from -0.1875 to 0.1875
- perceptron_rescaler: float32 [2048], replicated, may hold values from 0.1 to 1.9
- switching_projector: bfloat16 [2048, 5632], P('sp', 'tp'), may hold values from -0.125 to 0.125
- widening_projector: bfloat16 [2048, 5632], P('sp', 'tp'), may hold values from -0.125 to 0.125
- shrinking_projector: bfloat16 [5632, 2048], P('tp', 'sp'), may hold values from -0.078125 to 0.078125
Outputs:
- layer_out: bfloat16 [49152, 2048], P(('sp', 'tp'))
The draws below stay inside these ranges and needn't reach their ends.
Inputs may be any that keep to these rules, and one draw needn't show every extreme that they name: `passage_label_per_token`: document numbers never fall along the sequence; a document holds at most 6144 positions.
All inputs are finite; a program needn't handle non-finite values.
Results may differ from the reference program's by a relative error of at most 0.014.
Values may be sent and summed in bfloat16 or wider, within the bound.
A program may use at most 128 MiB of HBM per device.

```python
import math
import jax
import jax.numpy as jnp
import numpy as np
from jax import lax

D = 2048
HEADS = 8
DK = 64
DV = 128
FF = 5632
BLOCK = 64
TOK_DEV = 768
TOKENS = 49152
DOCS = 16
DOC_MOST = 6144
N_SP = 64
N_TP = 4


def draw_lapse_preactivation(key, part):
    base_key, block_key = jax.random.split(jax.random.fold_in(key, 11))
    width = HEADS * DK
    noise = jax.random.normal(base_key, (TOKENS, width), jnp.float32)
    shift = jax.random.uniform(block_key, (TOKENS // TOK_DEV, 1, width), jnp.float32, -0.7, 0.7)
    shaped = noise.reshape(TOKENS // TOK_DEV, TOK_DEV, width) + shift
    return shaped.reshape(TOKENS, width).astype(jnp.bfloat16)


def draw_lapse_shift_entries(key, part):
    pick_key, slow_key, fast_key = jax.random.split(jax.random.fold_in(key, 23), 3)
    slow = jax.random.randint(pick_key, (HEADS,), 0, 2) > 0
    slow_vals = jnp.log(TOKENS / 16.0) + jax.random.uniform(slow_key, (HEADS, DK), jnp.float32, -1.0, 0.5)
    fast_vals = jax.random.uniform(fast_key, (HEADS, DK), jnp.float32, -0.5, 1.5)
    return jnp.where(slow[:, None], slow_vals, fast_vals).reshape(HEADS * DK).astype(jnp.float32)


def draw_surplus_attenuation_terms(key, part):
    where_key, size_key = jax.random.split(jax.random.fold_in(key, 37))
    number = max(TOKENS // TOK_DEV, 4)
    spots = jax.random.randint(where_key, (number,), 0, TOKENS)
    depth = jnp.log(jax.random.uniform(size_key, (number,), jnp.float32, 0.5, 0.8))
    return jnp.zeros((TOKENS,), jnp.float32).at[spots].min(depth)


def steps_of(stream_key, shape, pieces, low, largest):
    def one(axis_at, shards_of):
        heights = jax.random.uniform(jax.random.fold_in(jax.random.fold_in(stream_key, 6), axis_at), (shards_of,), jnp.float32, low / len(pieces), largest / len(pieces))
        return jnp.repeat(jnp.exp(heights), shape[axis_at] // shards_of).reshape((-1,) + (1,) * (len(shape) - axis_at - 1))

    factor_of = one(*pieces[0])
    for cut in pieces[1:]:
        factor_of = factor_of * one(*cut)
    return factor_of


def profile(number_of, total, most, skew):
    portions = [(1 << 20) // math.isqrt(standing ** skew) + 1 for standing in range(2, number_of + 1)]
    surplus, holding = total - most - (number_of - 1), [1] * (number_of - 1)
    while surplus > 0:
        movable = [i for i in range(number_of - 1) if holding[i] < most]
        mass, remaining = sum([portions[i] for i in movable]), surplus
        for i in movable:
            extra = min(most - holding[i], max(1, remaining * portions[i] // mass), surplus)
            holding[i] = holding[i] + extra
            surplus = surplus - extra
    return np.array([most] + holding)


def uneven(rng, number_of, total, limit, skew):
    if number_of == 2:
        one = jax.random.randint(rng, (), max(1, total - limit), min(limit, total - 1) + 1)
        return jnp.stack([one, total - one])
    lengths = jnp.asarray(profile(number_of, total, limit, skew), jnp.int32)
    twos = (number_of - 1) // 2
    giver, receiver = lengths[1:1 + 2 * twos:2], lengths[2:2 + 2 * twos:2]
    slack = jnp.minimum(giver - 1, limit - receiver)
    passed = jax.random.randint(jax.random.fold_in(rng, 1), (twos,), 0, 1 << 20) % (slack + 1)
    lengths = lengths.at[1:1 + 2 * twos:2].set(giver - passed).at[2:2 + 2 * twos:2].set(receiver + passed)
    return lengths[jax.random.permutation(jax.random.fold_in(rng, 2), number_of)]


def scatter_about(own_key, shape, scale, reach, cuts=(), kind=jnp.bfloat16):
    drawn = scale * jax.random.normal(own_key, shape, jnp.float32)
    if cuts:
        drawn = drawn * steps_of(own_key, shape, cuts, -0.22, 0.18)
    return jnp.clip(drawn, -reach, reach).astype(kind)


def setup_inputs(seed: int = 0) -> dict:
    splits = jax.random.split(jax.random.key(seed), 16)
    skip_connection_stream = scatter_about(splits[0], (TOKENS, D), 1.0, 6.0, ((0, 64),))
    probing_vectors = scatter_about(splits[1], (TOKENS, HEADS * DK), 1.0, 6.0, ((0, 64), (1, 4)))
    addressing_vectors = scatter_about(splits[2], (TOKENS, HEADS * DK), 1.0, 6.0, ((0, 64), (1, 4)))
    mapped_payloads = scatter_about(splits[3], (TOKENS, HEADS * DV), 1.0, 6.0, ((0, 64), (1, 4)))
    emission_switch = scatter_about(splits[4], (TOKENS, HEADS * DV), 1.0, 6.0, ((0, 64), (1, 4)))
    lapse_preactivation = draw_lapse_preactivation(jax.random.fold_in(splits[15], 71), 0)
    lapse_shift_entries = draw_lapse_shift_entries(jax.random.fold_in(splits[15], 71), 0)
    surplus_attenuation_terms = draw_surplus_attenuation_terms(jax.random.fold_in(splits[15], 71), 0)
    passage_label_per_token = jnp.searchsorted(jnp.cumsum(uneven(splits[8], DOCS, TOKENS, DOC_MOST, 1)), jnp.arange(TOKENS), side="right").astype(jnp.int32)
    attention_group_rescaler = jnp.clip(1.0 + 0.18 * jax.random.normal(splits[9], (DV,), jnp.float32), 0.1, 1.9)
    emission_projector = scatter_about(splits[10], (HEADS * DV, D), (HEADS * DV) ** -0.5, 0.1875, ((0, 4),))
    perceptron_rescaler = jnp.clip(1.0 + 0.18 * jax.random.normal(splits[11], (D,), jnp.float32), 0.1, 1.9)
    switching_projector = scatter_about(splits[12], (D, FF), D ** -0.5, 0.125, ((0, 64), (1, 4)))
    widening_projector = scatter_about(splits[13], (D, FF), D ** -0.5, 0.125, ((0, 64), (1, 4)))
    shrinking_projector = scatter_about(splits[14], (FF, D), FF ** -0.5, 0.078125, ((0, 4), (1, 64)))
    return {"skip_connection_stream": skip_connection_stream, "probing_vectors": probing_vectors, "addressing_vectors": addressing_vectors, "mapped_payloads": mapped_payloads, "emission_switch": emission_switch, "lapse_preactivation": lapse_preactivation, "lapse_shift_entries": lapse_shift_entries, "surplus_attenuation_terms": surplus_attenuation_terms, "passage_label_per_token": passage_label_per_token, "attention_group_rescaler": attention_group_rescaler, "emission_projector": emission_projector, "perceptron_rescaler": perceptron_rescaler, "switching_projector": switching_projector, "widening_projector": widening_projector, "shrinking_projector": shrinking_projector}


eps = 1e-06
sharpness_factor = 16.0

def head_split(array, heads):
    return array.reshape(array.shape[0], heads, -1).transpose(1, 0, 2)

def rounded(value):
    return lax.optimization_barrier(value.astype(jnp.bfloat16)).astype(jnp.float32)

def block_pass(query_head_rows, key_heads, value_heads, decay_heads, documents, recurrent_state, last_doc, offset, span):
    heads, length, _ = query_head_rows.shape
    blocks = length // span

    def to_blocks(array):
        return array.reshape(heads, blocks, span, array.shape[-1]).transpose(1, 0, 2, 3)
    lower = jnp.tril(jnp.ones((span, span), dtype=bool))

    def step(carry, inputs):
        recurrent_state, last_doc, offset = carry
        query_block, key_blk, value_block, piece_attenuation, doc_blk = inputs
        cumulative_decay = jnp.cumsum(piece_attenuation, axis=1)
        previous_valid = (doc_blk == last_doc).astype(jnp.float32)
        cross_block_output = jnp.einsum('gfl,glm->gfm', query_block * jnp.exp(cumulative_decay), recurrent_state, precision=lax.Precision.HIGHEST) * previous_valid[None, :, None]
        spread = cumulative_decay[:, :, None, :] - cumulative_decay[:, None, :, :]
        same = (doc_blk[:, None] == doc_blk[None, :]) & lower
        weights = jnp.exp(jnp.where(same[None, :, :, None], spread, -jnp.inf))
        scores = jnp.einsum('hik,hjk,hijk->hij', query_block, key_blk, weights, precision=lax.Precision.HIGHEST)
        result = cross_block_output + jnp.einsum('hij,hjv->hiv', scores, value_block, precision=lax.Precision.HIGHEST)
        final_memory_summary = cumulative_decay[:, -1, :]
        last_valid = (doc_blk[-1] == last_doc).astype(jnp.float32)
        tail_ok = (doc_blk == doc_blk[-1]).astype(jnp.float32)
        decayed_keys = key_blk * jnp.exp(final_memory_summary[:, None, :] - cumulative_decay) * tail_ok[None, :, None]
        recurrent_state = recurrent_state * jnp.exp(final_memory_summary)[:, :, None] * last_valid + jnp.einsum('wrz,wrs->wzs', decayed_keys, value_block, precision=lax.Precision.HIGHEST)
        return ((recurrent_state, doc_blk[-1], offset + final_memory_summary), (result, cumulative_decay + offset[:, None, :]))
    carry, outputs = lax.scan(step, (recurrent_state, last_doc, offset), (to_blocks(query_head_rows), to_blocks(key_heads), to_blocks(value_heads), to_blocks(decay_heads), documents.reshape(blocks, span)))
    result, running_state = outputs
    result = result.transpose(1, 0, 2, 3).reshape(heads, length, -1)
    running_state = running_state.transpose(1, 0, 2, 3).reshape(heads, length, -1)
    return (carry[0], carry[2], result, running_state)

def reference(skip_connection_stream, probing_vectors, addressing_vectors, mapped_payloads, emission_switch, lapse_preactivation, lapse_shift_entries, surplus_attenuation_terms, passage_label_per_token, attention_group_rescaler, emission_projector, perceptron_rescaler, switching_projector, widening_projector, shrinking_projector):
    keeping_exponent = jax.nn.log_sigmoid(lapse_preactivation.astype(jnp.float32) + lapse_shift_entries[None, :]) / sharpness_factor + surplus_attenuation_terms[:, None]
    query_head_rows = head_split(probing_vectors.astype(jnp.float32) * DK ** (-0.5), HEADS)
    key_heads = head_split(addressing_vectors.astype(jnp.float32), HEADS)
    value_heads = head_split(mapped_payloads.astype(jnp.float32), HEADS)
    decay_heads = head_split(keeping_exponent, HEADS)
    zero_state = jnp.zeros((HEADS, DK, DV), jnp.float32)
    _, _, attn, _ = block_pass(query_head_rows, key_heads, value_heads, decay_heads, passage_label_per_token, zero_state, jnp.array(-1, jnp.int32), jnp.zeros((HEADS, DK), jnp.float32), BLOCK)
    normed_attn = attn * lax.rsqrt(lax.optimization_barrier(jnp.mean(attn * attn, axis=-1, keepdims=True)) + eps) * attention_group_rescaler
    flat = normed_attn.transpose(1, 0, 2).reshape(attn.shape[1], HEADS * DV)
    gated = (flat * jax.nn.silu(emission_switch.astype(jnp.float32))).astype(jnp.bfloat16)
    head_cols = HEADS * DV // N_TP
    ff_cols = FF // N_TP

    def rows_fn(index):
        start = (index * TOK_DEV).astype(jnp.int32)
        gated_rows = lax.dynamic_slice_in_dim(gated, start, TOK_DEV, 0)
        resid_rows = lax.dynamic_slice_in_dim(skip_connection_stream, start, TOK_DEV, 0)
        mixed = jnp.zeros((TOK_DEV, D), jnp.float32)
        for group in range(N_TP):
            mixed = mixed + rounded(jnp.dot(gated_rows[:, group * head_cols:(group + 1) * head_cols], emission_projector[group * head_cols:(group + 1) * head_cols], preferred_element_type=jnp.float32))
        first_resid = (resid_rows.astype(jnp.float32) + mixed).astype(jnp.bfloat16)
        wide = first_resid.astype(jnp.float32)
        normed = (wide * lax.rsqrt(lax.optimization_barrier(jnp.mean(wide * wide, axis=-1, keepdims=True)) + eps) * perceptron_rescaler).astype(jnp.bfloat16)
        gate = jnp.dot(normed, switching_projector, preferred_element_type=jnp.float32)
        upper = jnp.dot(normed, widening_projector, preferred_element_type=jnp.float32)
        hidden = (jax.nn.silu(gate) * upper).astype(jnp.bfloat16)
        ffn_out = jnp.zeros((TOK_DEV, D), jnp.float32)
        for group in range(N_TP):
            ffn_out = ffn_out + rounded(jnp.dot(hidden[:, group * ff_cols:(group + 1) * ff_cols], shrinking_projector[group * ff_cols:(group + 1) * ff_cols], preferred_element_type=jnp.float32))
        return (wide + 0.5 * ffn_out).astype(jnp.bfloat16)
    blocks_out = lax.map(rows_fn, jnp.arange(N_SP, dtype=jnp.int32))
    return blocks_out.reshape(N_SP * TOK_DEV, D)
```

```python
import functools

import jax
import jax.numpy as jnp
from jax import lax
from jax.experimental import pallas as pl
from jax.experimental.pallas import tpu as pltpu
from jax.sharding import Mesh
from jax.sharding import PartitionSpec as P

SP = ("sp_0", "sp_1", "sp_2")
SP_TP = ("sp_0", "sp_1", "sp_2", "tp")
EPS = 1e-06
SHARP = 16.0
B = 128
LEVELS = 7
AUX = 16
REACH = 8
LAG = 4
COLS = 256
MESH = pl.DeviceIdType.MESH
F32, BF16 = jnp.float32, jnp.bfloat16


def dot(a, b):
    return lax.dot_general(a, b, (((1,), (0,)), ((), ())), preferred_element_type=F32)


def dot_nt(a, b):
    return lax.dot_general(a, b, (((1,), (1,)), ((), ())), preferred_element_type=F32)


def dot_tn(a, b):
    return lax.dot_general(a, b, (((0,), (0,)), ((), ())), preferred_element_type=F32)


def kernel(
    sizes,
    skip_ref, q_ref, k_ref, v_ref, em_ref, lapse_ref, shift_ref, sur_ref, doc_ref, again_ref,
    we_ref, fgain_ref, wg_ref, wu_ref, wd_ref,
    out_ref,
    W, We, G, first, normed, hidden, part, rbuf, sbuf, carry_r, carry_s, ssq,
    oin, qp, ub, dc, gg_ref, tree, state,
    w_recv, w_dd, w_send, e_recv, e_dd, e_send, g_recv, g_send, c_recv, c_send, r_recv, r_send,
):
    Z, X, C, Y = sizes
    NSP = Z * X * C
    K = min(REACH, NSP - 1)
    T, D = skip_ref.shape
    R, FS = wg_ref.shape
    RW = we_ref.shape[0]
    NB = T // B
    HALF = T // 2
    OWN = T // Y
    NC = D // COLS
    z, x, c, y = (lax.axis_index(a) for a in SP_TP)
    s = 1 - 2 * c
    sp = (z * X + x) * C + c
    xn, zn, yn = (x + s + X) % X, (z + s + Z) % Z, (y + s + Y) % Y
    other = 1 - c

    def spdev(i):
        return {"sp_0": i // (X * C), "sp_1": (i // C) % X, "sp_2": i % C}

    barrier = pltpu.get_barrier_semaphore()
    peers = []
    for kk in range(1, K + 1):
        peers += [spdev((sp + kk) % NSP), spdev((sp + NSP - kk) % NSP)]
    peers += [{"sp_1": (x + 1) % X}, {"sp_1": (x + X - 1) % X}]
    peers += [{"sp_0": (z + 1) % Z}, {"sp_0": (z + Z - 1) % Z}]
    peers += [{"tp": (y + 1) % Y}, {"tp": (y + Y - 1) % Y}, {"sp_2": other}]
    for peer in peers:
        pl.semaphore_signal(barrier, inc=1, device_id=peer, device_id_type=MESH)
    pl.semaphore_wait(barrier, len(peers))

    def remote(src, dst, send, recv, dev):
        return pltpu.make_async_remote_copy(
            src_ref=src, dst_ref=dst, send_sem=send, recv_sem=recv, device_id=dev, device_id_type=MESH
        )

    own_w = (wg_ref, wu_ref, wd_ref)

    def slot(m, hx, hz):
        xs = (x + X - s * hx) % X if hx else x
        zs = (z + Z - s * hz) % Z if hz else z
        row = pl.multiple_of(((zs * X + xs) * C + c) * R, R)
        return W.at[m, pl.ds(row, R), :]

    def w_pass(m, hx, hz, way):
        here = slot(m, hx, hz)
        src = own_w[m] if hx == 0 and hz == 0 else here
        if way == "x":
            remote(src, here, w_send.at[m], w_recv.at[m, hx + 1, hz], {"sp_1": xn}).start()
        elif way == "z":
            remote(src, here, w_send.at[m], w_recv.at[m, hx, hz + 1], {"sp_0": zn}).start()
        else:
            remote(src, here, w_send.at[m], w_dd.at[m], {"sp_2": other}).start()

    def w_on(m, hx, hz):
        if m == 0:
            if hz < Z - 1:
                w_pass(m, hx, hz, "z")
            if hz == 0 and hx < X - 1:
                w_pass(m, hx, hz, "x")
        else:
            if hx == 0 and hz < Z - 1:
                w_pass(m, hx, hz, "z")
            if hx < X - 1:
                w_pass(m, hx, hz, "x")
        w_pass(m, hx, hz, "d")

    def w_event(m, hx, hz):
        here = slot(m, hx, hz)
        remote(here, here, w_send.at[m], w_recv.at[m, hx, hz], {"sp_2": other}).wait_recv()
        w_on(m, hx, hz)

    WAVES = X + Z - 2 + LAG

    def wave(n):
        for m in (1, 0, 2):
            k = n - LAG if m == 2 else n
            if k == 0:
                w_on(m, 0, 0)
            if k < 1:
                continue
            for hx in range(X):
                hz = k - hx
                if 0 <= hz < Z:
                    w_event(m, hx, hz)

    EP = RW // C // 2

    def e_rows(p, h):
        yb = (y + Y - s * h) % Y if h else y
        return pl.multiple_of(yb * RW + c * (RW // C) + p * EP, EP), c * (RW // C) + p * EP

    def e_on(p, h):
        row, mine = e_rows(p, h)
        here = We.at[pl.ds(row, EP), :]
        src = we_ref.at[pl.ds(pl.multiple_of(mine, EP), EP), :] if h == 0 else here
        if h < Y - 1:
            remote(src, here, e_send, e_recv.at[p, h + 1], {"tp": yn}).start()
        if h > 0:
            remote(src, here, e_send, e_dd, {"sp_2": other}).start()

    def e_event(p, h):
        row, _ = e_rows(p, h)
        here = We.at[pl.ds(row, EP), :]
        remote(here, here, e_send, e_recv.at[p, h], {"sp_2": other}).wait_recv()
        e_on(p, h)

    def g_on(r, h):
        yb = (y + Y - s * h) % Y if h else y
        here = G.at[yb, pl.ds(r * HALF, HALF), :]
        if h < Y - 1:
            remote(here, here, g_send, g_recv.at[r, h + 1], {"tp": yn}).start()

    def g_event(r, h):
        yb = (y + Y - s * h) % Y
        here = G.at[yb, pl.ds(r * HALF, HALF), :]
        remote(here, here, g_send, g_recv.at[r, h], {"sp_2": other}).wait_recv()
        g_on(r, h)

    wave(0)
    for p in range(2):
        e_on(p, 0)
    for m in range(3):
        row = pl.multiple_of(sp * R, R)
        W[m, pl.ds(row, R), :] = own_w[m][...]
    We[pl.ds(pl.multiple_of(y * RW, RW), RW), :] = we_ref[...]

    ti = lax.broadcasted_iota(jnp.int32, (B, 2 * B), 0)
    tt = lax.broadcasted_iota(jnp.int32, (B, 2 * B), 1) & (B - 1)
    for l in range(LEVELS):
        mid = ((ti >> (l + 1)) << (l + 1)) + (1 << l) - 1
        right = ((ti >> l) & 1) == 1
        among = (right & (tt > mid) & (tt <= ti)) | (~right & (tt > ti) & (tt <= mid))
        tree[l * B : (l + 1) * B, :] = among.astype(F32).astype(BF16)
    tree[LEVELS * B : (LEVELS + 1) * B, :] = (tt <= ti).astype(F32).astype(BF16)
    tree[(LEVELS + 1) * B : (LEVELS + 2) * B, :] = (tt > ti).astype(F32).astype(BF16)

    lane2 = lax.broadcasted_iota(jnp.int32, (B, 2 * B), 1)
    chan2 = lax.broadcasted_iota(jnp.int32, (B, 2 * B), 0)
    blockdiag = ((lane2 < B) == (chan2 < B // 2)).astype(F32)
    headrow = (lax.broadcasted_iota(jnp.int32, (B, B), 0) < B // 2).astype(F32)
    headlane = (lax.broadcasted_iota(jnp.int32, (B, B), 1) < B // 2).astype(F32)

    def rows_of(b):
        return pl.ds(pl.multiple_of(b * B, B), B)

    def down(row):
        return jnp.broadcast_to(row, (B, B)).T

    def block_docs(b):
        row = doc_ref[pl.ds(b, 1), :].astype(F32)
        col = down(row)
        return row, col, col[B - 1 : B, :]

    state[...] = jnp.zeros_like(state)
    ones2 = jnp.ones((2 * B, B), BF16)

    def decay_pass(b, carried):
        total, last = carried
        rows = rows_of(b)
        pre = lapse_ref[rows, :].astype(F32) + shift_ref[...]
        soft = jnp.minimum(pre, 0.0) - jnp.log1p(jnp.exp(-jnp.abs(pre)))
        g = jnp.maximum(soft / SHARP + down(sur_ref[pl.ds(b, 1), :]), -1e4)
        hi = g.astype(BF16)
        lo = (g - hi.astype(F32)).astype(BF16)
        gg = jnp.concatenate([hi, lo], axis=0)
        gg_ref[b] = gg
        sums = dot(tree[LEVELS * B :, :], gg)
        upto, after = sums[:B], sums[B:]
        col = jnp.exp(dot_tn(gg, ones2))
        dc[b] = col
        dcol, dlast = block_docs(b)[1:]
        tail = (dcol == dlast).astype(F32)
        keys = (k_ref[rows, :].astype(F32) * jnp.exp(after) * tail).astype(BF16)
        u = dot_tn(keys, v_ref[rows, :]) * blockdiag
        ub[b] = u
        qp[rows, :] = (q_ref[rows, :].astype(F32) * (0.125 * jnp.exp(upto))).astype(BF16)
        same = (dlast == last).astype(F32)
        keep = col * same
        state[...] = state[...] * jnp.concatenate([keep, keep], axis=1) + u
        return total + upto[B - 1 : B, :], dlast

    total, last = lax.fori_loop(
        0, NB, decay_pass, (jnp.zeros((1, B), F32), jnp.full((1, B), -1.0, F32))
    )
    whole = state[...]
    carry_s[0:B, :] = (whole[:, :B] * headrow + whole[:, B:] * (1.0 - headrow)).astype(BF16)
    t_hi = total.astype(BF16).astype(F32)
    t_mid = (total - t_hi).astype(BF16).astype(F32)
    t_lo = total - t_hi - t_mid
    ri = lax.broadcasted_iota(jnp.int32, (AUX, B), 0)
    aux = jnp.where(ri == 0, t_hi, 0.0)
    aux = jnp.where(ri == 1, t_mid, aux)
    aux = jnp.where(ri == 2, t_lo, aux)
    aux = jnp.where(ri == 3, last, aux)
    carry_s[B : B + AUX, :] = aux.astype(BF16)

    ii = lax.broadcasted_iota(jnp.int32, (2 * B, B), 0) & (B - 1)
    jj = lax.broadcasted_iota(jnp.int32, (2 * B, B), 1)
    xx = ii ^ jj

    def inner_pass(b, _):
        rows = rows_of(b)
        gg = gg_ref[b]
        q = q_ref[rows, :].astype(F32) * 0.125
        key = k_ref[rows, :].astype(F32)
        qq = jnp.concatenate([q * headlane, q * (1.0 - headlane)], axis=0)
        scores = jnp.where(xx == 0, dot_nt(qq.astype(BF16), k_ref[rows, :]), 0.0)
        sums = dot(tree[: LEVELS * B, :], gg)
        for l in range(LEVELS):
            e = jnp.exp(sums[l * B : (l + 1) * B])
            sl = dot_nt((qq * jnp.concatenate([e, e], axis=0)).astype(BF16), (key * e).astype(BF16))
            mine = ((xx >> l) == 1) & (((ii >> l) & 1) == 1)
            scores = jnp.where(mine, sl, scores)
        drow, dcol = block_docs(b)[:2]
        alike = (dcol == drow).astype(F32)
        scores = scores * jnp.concatenate([alike, alike], axis=0)
        sv = dot(scores.astype(BF16), v_ref[rows, :])
        oin[rows, :] = jnp.concatenate([sv[:B, :B], sv[B:, B:]], axis=1)
        return _

    for kk in range(1, K + 1):
        remote(carry_s, carry_r.at[kk - 1], c_send, c_recv.at[kk - 1], spdev((sp + kk) % NSP)).start()

    third = max(NB * 2 // 3, 1)
    lax.fori_loop(0, third, inner_pass, 0)
    wave(1)
    e_event(0, 1)
    lax.fori_loop(third, NB, inner_pass, 0)

    for kk in range(1, K + 1):
        remote(carry_s, carry_r.at[kk - 1], c_send, c_recv.at[kk - 1], {"sp_2": other}).wait_recv()
    aux_all = jnp.concatenate([carry_r[kk, B : B + AUX, :] for kk in range(K)], axis=0)
    zi = lax.broadcasted_iota(jnp.int32, (K * AUX, B), 0)
    last_in = carry_r[0, B : B + AUX, :].astype(F32)[3:4, :]
    come = jnp.zeros((B, B), F32)
    for kk in range(1, K + 1):
        piece = carry_r[kk - 1, 0:B, :].astype(F32)
        if kk > 1:
            pick = (((zi & (AUX - 1)) < 3) & (zi < (kk - 1) * AUX)).astype(F32).astype(BF16)
            piece = piece * jnp.exp(dot_tn(aux_all, pick))
        its = carry_r[kk - 1, B : B + AUX, :].astype(F32)[3:4, :]
        good = jnp.where(its == last_in, 1.0, 0.0) * jnp.where(sp >= kk, 1.0, 0.0)
        come = come + piece * good
    state[...] = jnp.concatenate([come * headrow, come * (1.0 - headrow)], axis=1)
    last_in = jnp.where(sp >= 1, last_in, -1.0)
    e_event(1, 1)

    def outer_pass(b, last):
        rows = rows_of(b)
        dcol, dlast = block_docs(b)[1:]
        reach = (dcol == last).astype(F32)
        st = state[...]
        o = oin[rows, :] + dot(qp[rows, :], st.astype(BF16)) * jnp.concatenate([reach, reach], axis=1)
        keep = dc[b] * (dlast == last).astype(F32)
        state[...] = st * jnp.concatenate([keep, keep], axis=1) + ub[b]
        em = em_ref[rows, :].astype(F32)
        gate = em / (1.0 + jnp.exp(-em))
        halves = []
        for h in range(2):
            oh = o[:, h * B : (h + 1) * B]
            scale = lax.rsqrt(jnp.mean(oh * oh, axis=-1, keepdims=True) + EPS)
            halves.append(oh * scale * again_ref[...] * gate[:, h * B : (h + 1) * B])
        G[y, rows, :] = jnp.concatenate(halves, axis=1).astype(BF16)
        return dlast

    last = lax.fori_loop(0, NB // 2, outer_pass, last_in)
    g_on(0, 0)
    last = lax.fori_loop(NB // 2, NB, outer_pass, last)
    g_on(1, 0)

    done = [1]

    def next_wave():
        if done[0] < WAVES:
            done[0] += 1
            wave(done[0])

    next_wave()
    for h in range(1, Y):
        for r in range(2):
            if h > 1:
                e_event(r, h)
        next_wave()
        for r in range(2):
            g_event(r, h)

    remote(We.at[pl.ds(0, (Y - 1) * RW // C)], We.at[pl.ds(0, (Y - 1) * RW // C)], e_send, e_dd, {"sp_2": other}).wait_recv()
    NW = 512 if D % 512 == 0 else COLS

    def mix_half(r):
        rows = pl.ds(r * HALF, HALF)
        ssq[...] = jnp.zeros_like(ssq)

        def columns(n, _):
            cols = pl.ds(pl.multiple_of(n * NW, NW), NW)
            left = jnp.concatenate([G[yb, rows, :] for yb in range(Y)], axis=1)
            mixed = dot(left, We[:, cols])
            fr = (skip_ref[rows, cols].astype(F32) + mixed).astype(BF16)
            first[rows, cols] = fr
            wide = fr.astype(F32)
            sq = wide * wide
            ssq[...] += sum(sq[:, i * 128 : (i + 1) * 128] for i in range(NW // 128))
            return _

        lax.fori_loop(0, D // NW, columns, 0)
        ssq[...] = jnp.broadcast_to(
            lax.rsqrt(jnp.sum(ssq[...], axis=-1, keepdims=True) / D + EPS), ssq.shape
        )

        def scaled(i, _):
            mine = pl.ds(pl.multiple_of(r * HALF + i * 64, 64), 64)
            sc = ssq[pl.ds(pl.multiple_of(i * 64, 64), 64), :]
            for n in range(D // 128):
                cols = slice(n * 128, (n + 1) * 128)
                normed[mine, cols] = (first[mine, cols].astype(F32) * sc * fgain_ref[:, cols]).astype(BF16)
            return _

        lax.fori_loop(0, HALF // 64, scaled, 0)

    mix_half(0)
    next_wave()
    mix_half(1)
    while done[0] < X + Z - 2:
        next_wave()

    def all_here(m):
        n = pl.ds(0, R * X * Z)
        remote(W.at[m, n, :], W.at[m, n, :], w_send.at[m], w_dd.at[m], {"sp_2": other}).wait_recv()

    all_here(0)
    all_here(1)

    def hidden_cols(n, _):
        cols = pl.ds(pl.multiple_of(n * 128, 128), 128)
        both = dot(normed[...], jnp.concatenate([W[0, :, cols], W[1, :, cols]], axis=1))
        gate = both[:, :128]
        hidden[:, cols] = (gate / (1.0 + jnp.exp(-gate)) * both[:, 128:]).astype(BF16)
        return _

    tiles = FS // 128
    left_over = max(WAVES - done[0], 1)
    at = 0
    for i in range(left_over):
        to = tiles * (i + 1) // left_over
        lax.fori_loop(at, to, hidden_cols, 0)
        at = to
        next_wave()
    all_here(2)

    def block_of(t):
        return pl.ds(pl.multiple_of(((y + 2 * Y - s * t) % Y) * OWN, OWN), OWN)

    def send_on(t, j):
        remote(sbuf.at[t, j], rbuf.at[t, j], r_send, r_recv.at[t, j], {"tp": yn}).start()

    def arrive(t, j):
        remote(sbuf.at[t, j], rbuf.at[t, j], r_send, r_recv.at[t, j], {"sp_2": other}).wait_recv()

    def reduce_step(i, same):
        @pl.when(i < NC)
        def _():
            rows = pl.ds(pl.multiple_of(i * COLS, COLS), COLS)
            part[i] = dot_nt(hidden[...], W[2, rows, :])
            sbuf[0, i] = part[i, block_of(1), :].astype(BF16)
            send_on(0, i)

        for t in range(1, Y):
            j = i - LAG * t

            @pl.when((j >= 0) & (j < NC))
            def _():
                arrive(t - 1, j)
                total = rbuf[t - 1, j].astype(F32) + part[j, block_of(t + 1), :]
                if t < Y - 1:
                    sbuf[t, j] = total.astype(BF16)
                    send_on(t, j)
                else:
                    cols = pl.ds(pl.multiple_of(j * COLS, COLS), COLS)
                    own = first[block_of(0), cols].astype(F32)
                    out_ref[:, cols] = (own + 0.5 * total).astype(BF16)

        return same

    lax.fori_loop(0, NC + LAG * (Y - 1), reduce_step, 0)

    for m in range(3):
        n = pl.ds(0, R * (2 * X * Z - 1))
        remote(W.at[m, n, :], W.at[m, n, :], w_send.at[m], w_dd.at[m], {"sp_2": other}).wait_send()
    n = pl.ds(0, EP * 2 * 2 * (Y - 1))
    remote(We.at[n], We.at[n], e_send, e_dd, {"sp_2": other}).wait_send()
    n = pl.ds(0, Y - 1)
    remote(G.at[n], G.at[n], g_send, g_recv.at[0, 0], {"sp_2": other}).wait_send()
    n = pl.ds(0, K)
    remote(carry_r.at[n], carry_r.at[n], c_send, c_recv.at[0], {"sp_2": other}).wait_send()
    remote(sbuf, sbuf, r_send, r_recv.at[0, 0], {"sp_2": other}).wait_send()


def per_device(
    sizes,
    skip_connection_stream,
    probing_vectors,
    addressing_vectors,
    mapped_payloads,
    emission_switch,
    lapse_preactivation,
    lapse_shift_entries,
    surplus_attenuation_terms,
    passage_label_per_token,
    attention_group_rescaler,
    emission_projector,
    perceptron_rescaler,
    switching_projector,
    widening_projector,
    shrinking_projector,
):
    Z, X, C, Y = sizes
    T, D = skip_connection_stream.shape
    R, FS = switching_projector.shape
    RW = emission_projector.shape[0]
    NB = T // B
    K = min(REACH, Z * X * C - 1)
    NC = D // COLS
    operands = (
        skip_connection_stream,
        probing_vectors,
        addressing_vectors,
        mapped_payloads,
        emission_switch,
        lapse_preactivation,
        lapse_shift_entries.reshape(1, B),
        surplus_attenuation_terms.reshape(NB, B),
        passage_label_per_token.reshape(NB, B),
        attention_group_rescaler.reshape(1, B),
        emission_projector,
        perceptron_rescaler.reshape(1, D),
        switching_projector,
        widening_projector,
        shrinking_projector.T,
    )
    dma = pltpu.SemaphoreType.DMA
    return pl.pallas_call(
        functools.partial(kernel, sizes),
        out_shape=jax.ShapeDtypeStruct((T // Y, D), BF16),
        in_specs=[pl.BlockSpec(memory_space=pltpu.VMEM)] * len(operands),
        out_specs=pl.BlockSpec(memory_space=pltpu.VMEM),
        scratch_shapes=[
            pltpu.VMEM((3, D, FS), BF16),
            pltpu.VMEM((Y * RW, D), BF16),
            pltpu.VMEM((Y, T, 2 * B), BF16),
            pltpu.VMEM((T, D), BF16),
            pltpu.VMEM((T, D), BF16),
            pltpu.VMEM((T, FS), BF16),
            pltpu.VMEM((NC, T, COLS), F32),
            pltpu.VMEM((Y - 1, NC, T // Y, COLS), BF16),
            pltpu.VMEM((Y - 1, NC, T // Y, COLS), BF16),
            pltpu.VMEM((K, B + AUX, B), BF16),
            pltpu.VMEM((B + AUX, B), BF16),
            pltpu.VMEM((T // 2, 128), F32),
            pltpu.VMEM((T, 2 * B), F32),
            pltpu.VMEM((T, B), BF16),
            pltpu.VMEM((NB, B, 2 * B), F32),
            pltpu.VMEM((NB, B, B), F32),
            pltpu.VMEM((NB, 2 * B, B), BF16),
            pltpu.VMEM(((LEVELS + 2) * B, 2 * B), BF16),
            pltpu.VMEM((B, 2 * B), F32),
            dma((3, X, Z)),
            dma((3,)),
            dma((3,)),
            dma((2, Y)),
            dma(()),
            dma(()),
            dma((2, Y)),
            dma(()),
            dma((K,)),
            dma(()),
            dma((Y - 1, NC)),
            dma(()),
        ],
        compiler_params=pltpu.CompilerParams(
            collective_id=0, has_side_effects=True, vmem_limit_bytes=67043328
        ),
        name="layer",
    )(*operands)


def solution(mesh):
    sp, tp = mesh.shape["sp"], mesh.shape["tp"]
    sizes = (sp // 8, 4, 2, tp)
    torus = Mesh(mesh.devices.reshape(sizes), SP_TP)
    in_specs = (
        P(SP, None),
        P(SP, "tp"),
        P(SP, "tp"),
        P(SP, "tp"),
        P(SP, "tp"),
        P(SP, "tp"),
        P("tp"),
        P(SP),
        P(SP),
        P(),
        P("tp", None),
        P(),
        P(SP, "tp"),
        P(SP, "tp"),
        P("tp", SP),
    )
    return jax.shard_map(
        functools.partial(per_device, sizes),
        mesh=torus,
        in_specs=in_specs,
        out_specs=P(SP_TP, None),
        check_vma=False,
    )
```
